32 devices in a mesh: grp: 2 (over y), ep: 4 (over z), tp: 4 (over x, core).
Axes of the slice: x: 2, y: 2, z: 4, core: 2. Of those that a mesh axis runs over, the one named last changes fastest.
Arguments:
- queries: bfloat16 [1024, 16, 128], P(('grp', 'ep'), 'tp'), parts along dimension 0, may hold values from -6 to 6
- key_vectors: bfloat16 [1024, 16, 128], P(('grp', 'ep'), 'tp'), parts along dimension 0, may hold values from -6 to 6
- values: bfloat16 [1024, 16, 128], P(('grp', 'ep'), 'tp'), parts along dimension 0, may hold values from -6 to 6
- forget_cum: float32 [1024, 16], P('grp', 'tp'), parts along dimension 0, may hold values from -90 to 0, as said below
- query_gain: float32 [128], replicated, may hold values from 0.1 to 5.5
- key_gain: float32 [128], replicated, may hold values from 0.1 to 5.5
- tokens: bfloat16 [4096, 4096], P(('grp', 'ep', 'tp')), parts along dimension 0, may hold values from -6 to 6
- norm_gain: float32 [4096], replicated, may hold values from 0.1 to 1.9
- routes: int32 [4096, 2], P(('grp', 'ep', 'tp')), parts along dimension 0, may hold values from 0 to 127, all different within a row; in each aligned block of 128 rows (0 to 127, 128 to 255, ...) at most 2 rows name the same one
- route_weights: float32 [4096, 2], P(('grp', 'ep', 'tp')), parts along dimension 0, may hold values from 0.3 to 1.2
- expert_gate: bfloat16 [128, 4096, 384], P(('ep', 'tp')), may hold values from -0.09375 to 0.09375
- expert_up: bfloat16 [128, 4096, 384], P(('ep', 'tp')), may hold values from -0.09375 to 0.09375
- expert_down: bfloat16 [128, 384, 4096], P(('ep', 'tp')), may hold values from -0.3125 to 0.3125
- shared_gate: bfloat16 [4096, 192], P(None, 'tp'), may hold values from -0.09375 to 0.09375
- shared_up: bfloat16 [4096, 192], P(None, 'tp'), may hold values from -0.09375 to 0.09375
- shared_down: bfloat16 [192, 4096], P('tp'), may hold values from -0.4375 to 0.4375
Outputs:
- attended: bfloat16 [1024, 16, 128], P(('grp', 'ep'), 'tp'), parts along dimension 0
- routed_output: bfloat16 [4096, 4096], P(('grp', 'ep', 'tp')), parts along dimension 0
The draws below stay inside these ranges and needn't reach their ends.
There are 2 independent parts, one for each index of `grp`. The reference program is written for one: setup_inputs(seed, part) draws one part's arguments, and reference() takes and returns one part's arrays. A program takes and returns all parts, laid end to end along the dimension named above; an argument that names none is the same for every part. Nothing has to cross between parts.
Inputs may be any that keep to these rules, and one draw needn't show every extreme that they name: `routes`: each row names 2 different experts; the rows of one device name every expert exactly 2 times. `forget_cum`: never rises from one position to the next.
All inputs are finite; a program needn't handle non-finite values.
Results may differ from the reference program's by a relative error of at most 0.007.
The reference program's roundings to bfloat16 on the way count: a program that leaves them out, or rounds other values in their place, can miss the bound.
Values may be sent and summed in bfloat16 or wider, within the bound.
No kernel may reach another device: no remote copies, remote signals or barrier semaphores. Data moves between devices by JAX's collectives and lax.ppermute only.
A program may use at most 128 MiB of HBM per device.

```python
import math
import jax
import jax.numpy as jnp
import numpy as np
from jax import lax

D = 4096
HEADS = 16
HD = 128
EXPERTS = 128
EF = 384
SF = 192
TOP_K = 2
TOKENS_PER_SHARD = 128
TOK_B = 128
CAP = 2
SEQUENCE_LENGTH = 512
TOKENS_B = 2048
N_EP = 4
N_TP = 4


def query_key_pair(key):
    query_base = jnp.clip(jax.random.normal(jax.random.fold_in(key, 701), (SEQUENCE_LENGTH, HEADS, HD), jnp.float32), -6.0, 6.0)
    key_base = jnp.clip(jax.random.normal(jax.random.fold_in(key, 702), (SEQUENCE_LENGTH, HEADS, HD), jnp.float32), -6.0, 6.0)
    return (query_base, key_base)


def draw_queries(key, part):
    return query_key_pair(key)[0].astype(jnp.bfloat16)


def draw_key_vectors(key, part):
    return query_key_pair(key)[1].astype(jnp.bfloat16)


def gain_sample(key):
    return 1.0 + jnp.clip(0.18 * jax.random.normal(key, (HD,), jnp.float32), -0.9, 0.9)


def draw_query_gain(key, part):
    return gain_sample(jax.random.fold_in(key, 801))


def draw_key_gain(key, part):
    return gain_sample(jax.random.fold_in(key, 802))


def draw_forget_cum(key, part):
    order = jax.random.permutation(jax.random.fold_in(key, 901), HEADS)
    gentle_decay = (order < HEADS // 2).astype(jnp.float32)
    totals = jnp.exp(jax.random.uniform(jax.random.fold_in(key, 902), (HEADS,), jnp.float32, jnp.log(0.3), jnp.log(1.0))) / SEQUENCE_LENGTH
    quick = jnp.exp(jax.random.uniform(jax.random.fold_in(key, 903), (HEADS,), jnp.float32, jnp.log(1.0 / 60.0), jnp.log(1.0 / 25.0)))
    decay_speed = gentle_decay * totals + (1.0 - gentle_decay) * quick
    block_multiplier = jnp.exp(jax.random.uniform(jax.random.fold_in(key, 904), (SEQUENCE_LENGTH // TOKENS_PER_SHARD,), jnp.float32, jnp.log(0.35), jnp.log(2.8)))
    jagged_profile = jax.random.uniform(jax.random.fold_in(key, 905), (SEQUENCE_LENGTH, HEADS), jnp.float32, 0.5, 1.5)
    position_indices = jnp.arange(SEQUENCE_LENGTH)
    spike_position = jax.random.randint(jax.random.fold_in(key, 906), (3,), 0, SEQUENCE_LENGTH)
    spike_magnitude = jax.random.uniform(jax.random.fold_in(key, 907), (3,), jnp.float32, 0.22, 0.69)
    forget_spike = jnp.sum(jnp.where(position_indices[:, None] == spike_position[None, :], spike_magnitude[None, :], 0.0), axis=1)
    forget_logarithm = -(decay_speed[None, :] * jnp.repeat(block_multiplier, TOKENS_PER_SHARD)[:, None] * jagged_profile) - forget_spike[:, None] * gentle_decay[None, :]
    return jnp.cumsum(forget_logarithm, axis=0)


def block_levels(stream_key, shape, shards, least, top_value):
    gain, own = 1.0, jax.random.fold_in(stream_key, 6)
    for dim, parts in shards:
        draws = jnp.exp(jax.random.uniform(jax.random.fold_in(own, dim), (parts,), jnp.float32, least / len(shards), top_value / len(shards)))
        gain = gain * jnp.repeat(draws, shape[dim] // parts).reshape([-1 if axis == dim else 1 for axis in range(len(shape))])
    return gain


def deal_out(own_key, own, number, rows, amount, top, most, lean):
    order = jax.random.permutation(own_key, amount)
    heavy_load, usual = portions_of(amount, rows * top, most, lean, True), portions_of(amount, rows * top, most, lean, False)
    places = jnp.arange(amount)

    def named(sizes, rotation):
        used = int((sizes > 0).sum())
        fixed = max(1, used // 4)
        passed = fixed + (places - fixed + rotation * (used - fixed)) % max(1, amount - fixed)
        return jnp.zeros((amount,), jnp.int32).at[order[jnp.where(places < fixed, places, passed)]].set(jnp.asarray(sizes, jnp.int32))

    sizes = jnp.where(number % 4 == 0, named(heavy_load, number // 4), named(usual, number - number // 4 - 1))
    mixed = jax.random.permutation(jax.random.fold_in(own, 3), amount)
    source_of, taker = mixed[0:amount // 2 * 2:2], mixed[1:amount // 2 * 2:2]
    margin = jnp.minimum(sizes[source_of] - 1, most - sizes[taker]) // 2
    margin = jnp.where((source_of == order[0]) | (taker == order[0]) | (sizes[taker] == 0), 0, jnp.maximum(margin, 0))
    passed = jax.random.randint(jax.random.fold_in(own, 4), (amount // 2,), 0, 1 << 20) % (margin + 1)
    sizes = sizes.at[source_of].add(-passed).at[taker].add(passed)
    items = jnp.searchsorted(jnp.cumsum(sizes), jnp.arange(rows * top), side="right").astype(jnp.int32)
    grid = items.reshape(top, rows).T
    grid = grid[jax.random.permutation(jax.random.fold_in(own, 1), rows)]
    rotation = jax.random.randint(jax.random.fold_in(own, 2), (rows, 1), 0, top)
    return jnp.take_along_axis(grid, (jnp.arange(top)[None, :] + rotation) % top, axis=1)


def portions_of(number_of, total, limit, skew, full):
    loads = [(1 << 20) // math.isqrt(grade ** skew) + 1 for grade in range(1, number_of + 1)]
    largest = limit if full else min(limit, max(-(-total // number_of), total * loads[0] // sum(loads)))
    least = 1 if total - largest >= number_of - 1 else 0
    counts, surplus = [largest] + [least] * (number_of - 1), total - largest - least * (number_of - 1)
    while surplus > 0:
        movable = [i for i in range(1, number_of) if counts[i] < largest] or [i for i in range(1, number_of) if counts[i] < limit]
        mass, budget = sum([loads[i] for i in movable]), surplus
        for i in movable:
            addition = min(limit - counts[i], max(1, budget * loads[i] // mass), surplus)
            counts[i] = counts[i] + addition
            surplus = surplus - addition
    return np.array(counts)


def scatter_about(key, dims, width, most, shards=(), held_as=jnp.bfloat16):
    level = block_levels(key, dims, shards, -0.22, 0.18) if shards else 1.0
    drawn = jax.random.normal(key, dims, jnp.float32) * width * level
    return jnp.minimum(jnp.maximum(drawn, -most), most).astype(held_as)


def setup_inputs(seed: int = 0, part: int = 0) -> dict:
    streams_of = jax.random.split(jax.random.key(seed), 17)
    part_keys = jax.random.split(jax.random.fold_in(streams_of[16], part), 17)
    queries = draw_queries(jax.random.fold_in(jax.random.fold_in(streams_of[16], part), 71), part)
    key_vectors = draw_key_vectors(jax.random.fold_in(jax.random.fold_in(streams_of[16], part), 71), part)
    values = scatter_about(part_keys[2], (SEQUENCE_LENGTH, HEADS, HD), 1.0, 6.0, ((0, 4), (1, 4)))
    forget_cum = draw_forget_cum(jax.random.fold_in(jax.random.fold_in(streams_of[16], part), 71), part)
    query_gain = draw_query_gain(jax.random.fold_in(streams_of[16], 71), part)
    key_gain = draw_key_gain(jax.random.fold_in(streams_of[16], 71), part)
    tokens = scatter_about(part_keys[6], (TOKENS_B, D), 1.0, 6.0, ((0, 16),))
    norm_gain = jnp.clip(1.0 + 0.18 * jax.random.normal(streams_of[7], (D,), jnp.float32), 0.1, 1.9)
    routes_keys = jax.random.split(jax.random.fold_in(part_keys[8], 1), TOKENS_B // TOK_B)
    routes_turns = jax.random.permutation(jax.random.fold_in(part_keys[8], 3), TOKENS_B // TOK_B)
    routes = jax.vmap(lambda own, number: deal_out(jax.random.fold_in(part_keys[8], 2), own, number, TOK_B, EXPERTS, TOP_K, CAP, 0))(routes_keys, routes_turns).reshape((TOKENS_B, TOP_K))
    route_weights = jnp.clip(0.3 + 0.90000004 * jax.random.uniform(part_keys[9], (TOKENS_B, TOP_K), jnp.float32) ** block_levels(part_keys[9], (TOKENS_B, TOP_K), ((0, 16),), -0.2, 0.2), 0.3, 1.2)
    expert_gate = scatter_about(streams_of[10], (EXPERTS, D, EF), D ** -0.5, 0.09375, ((0, 16),))
    expert_up = scatter_about(streams_of[11], (EXPERTS, D, EF), D ** -0.5, 0.09375, ((0, 16),))
    expert_down = scatter_about(streams_of[12], (EXPERTS, EF, D), EF ** -0.5, 0.3125, ((0, 16),))
    shared_gate = scatter_about(streams_of[13], (D, SF), D ** -0.5, 0.09375, ((1, 4),))
    shared_up = scatter_about(streams_of[14], (D, SF), D ** -0.5, 0.09375, ((1, 4),))
    shared_down = scatter_about(streams_of[15], (SF, D), SF ** -0.5, 0.4375, ((0, 4),))
    return {"queries": queries, "key_vectors": key_vectors, "values": values, "forget_cum": forget_cum, "query_gain": query_gain, "key_gain": key_gain, "tokens": tokens, "norm_gain": norm_gain, "routes": routes, "route_weights": route_weights, "expert_gate": expert_gate, "expert_up": expert_up, "expert_down": expert_down, "shared_gate": shared_gate, "shared_up": shared_up, "shared_down": shared_down}


def rms_rows(row_values, gain_vector):
    widened = row_values.astype(jnp.float32)
    inverse = lax.rsqrt(lax.optimization_barrier(jnp.mean(widened * widened, axis=-1, keepdims=True)) + 1e-06)
    return (widened * inverse * gain_vector.astype(jnp.float32)).astype(jnp.bfloat16)

def attention(queries, key_vectors, values, forget_cum, query_gain, key_gain):
    query_norm = lax.optimization_barrier(rms_rows(queries, query_gain)).astype(jnp.float32)
    key_norm = lax.optimization_barrier(rms_rows(key_vectors, key_gain)).astype(jnp.float32)
    value_wide = values.astype(jnp.float32)
    length = queries.shape[0]
    block_rows = 512 if length % 512 == 0 else length
    scale_factor = queries.shape[2] ** (-0.5)
    outputs = []
    for first_row in range(0, length, block_rows):
        stop_row = first_row + block_rows
        scores = jnp.einsum('qhd,khd->hqk', query_norm[first_row:stop_row], key_norm[:stop_row]) * scale_factor
        scores = scores + forget_cum[first_row:stop_row].T[:, :, None] - forget_cum[:stop_row].T[:, None, :]
        allowed = (jnp.arange(stop_row)[None, :] <= jnp.arange(first_row, stop_row)[:, None])[None]
        scores = jnp.where(allowed, scores, -jnp.inf)
        row_max = lax.optimization_barrier(jnp.max(scores, axis=2, keepdims=True))
        weights = jnp.exp(scores - row_max)
        denominator = lax.optimization_barrier(jnp.sum(weights, axis=2))
        probabilities = lax.optimization_barrier(weights.astype(jnp.bfloat16)).astype(jnp.float32)
        mixed_rows = jnp.einsum('hqk,khd->hqd', probabilities, value_wide[:stop_row]) / denominator[:, :, None]
        outputs.append(mixed_rows.transpose(1, 0, 2))
    return jnp.concatenate(outputs, axis=0).astype(jnp.bfloat16)

def mixture(tokens, norm_gain, routes, route_weights, expert_gate, expert_up, expert_down, shared_gate, shared_up, shared_down):
    normed = rms_rows(tokens, norm_gain)
    row_total = tokens.shape[0]
    shared_hidden = (jax.nn.silu(jnp.dot(normed, shared_gate, preferred_element_type=jnp.float32)) * jnp.dot(normed, shared_up, preferred_element_type=jnp.float32)).astype(jnp.bfloat16)
    part_width = shared_down.shape[0] // N_TP
    shared_sum = jnp.zeros((row_total, tokens.shape[1]), jnp.float32)
    for block_index in range(N_TP):
        low = block_index * part_width
        partial_value = jnp.dot(shared_hidden[:, low:low + part_width], shared_down[low:low + part_width], preferred_element_type=jnp.float32)
        shared_sum = shared_sum + lax.optimization_barrier(partial_value.astype(jnp.bfloat16)).astype(jnp.float32)
    shared_out = shared_sum.astype(jnp.bfloat16)
    block_count = N_EP * N_TP
    per_block = routes.reshape(block_count, -1)
    choices_per = per_block.shape[1]
    token_index = (jnp.arange(block_count)[:, None] * (choices_per // TOP_K) + jnp.arange(choices_per)[None, :] // TOP_K).astype(jnp.int32)
    weight_table = route_weights.reshape(block_count, -1)
    one_hot = (per_block[:, :, None] == jnp.arange(EXPERTS)[None, None, :]).astype(jnp.int32)
    slot_rank = lax.optimization_barrier(jnp.sum((jnp.cumsum(one_hot, axis=1) - one_hot) * one_hot, axis=2))

    def one_expert(running_sum, expert_index):
        chosen = per_block == expert_index
        placed = chosen[:, :, None] & (slot_rank[:, :, None] == jnp.arange(CAP)[None, None, :])
        row_ids = lax.optimization_barrier(jnp.sum(jnp.where(placed, token_index[:, :, None], 0), axis=1)).reshape(-1).astype(jnp.int32)
        slot_weight = lax.optimization_barrier(jnp.sum(jnp.where(placed, weight_table[:, :, None], 0.0), axis=1)).reshape(-1)
        picked = normed[row_ids]
        gate_values = jnp.dot(picked, expert_gate[expert_index], preferred_element_type=jnp.float32)
        upward = jnp.dot(picked, expert_up[expert_index], preferred_element_type=jnp.float32)
        hidden = (jax.nn.silu(gate_values) * upward).astype(jnp.bfloat16)
        produced = jnp.dot(hidden, expert_down[expert_index], preferred_element_type=jnp.float32).astype(jnp.bfloat16)
        produced = lax.optimization_barrier(produced).astype(jnp.float32)
        return (running_sum.at[row_ids].add(slot_weight[:, None] * produced), None)
    routed, _ = lax.scan(one_expert, jnp.zeros((row_total, tokens.shape[1]), jnp.float32), jnp.arange(EXPERTS).astype(jnp.int32))
    return (shared_out.astype(jnp.float32) + routed).astype(jnp.bfloat16)

def reference(queries, key_vectors, values, forget_cum, query_gain, key_gain, tokens, norm_gain, routes, route_weights, expert_gate, expert_up, expert_down, shared_gate, shared_up, shared_down):
    attended = attention(queries, key_vectors, values, forget_cum, query_gain, key_gain)
    routed_output = mixture(tokens, norm_gain, routes, route_weights, expert_gate, expert_up, expert_down, shared_gate, shared_up, shared_down)
    return (attended, routed_output)
```

```python
import functools

import jax
import jax.numpy as jnp
from jax import lax
from jax.experimental import pallas as pl
from jax.experimental.pallas import tpu as pltpu
from jax.sharding import PartitionSpec as P

CAP = 2
GROUP = ("ep", "tp")
CHUNKS = 1
EARLY_SHARED = False


def power_of_two(n):
    return n & (n - 1) == 0


def rms_rows(row_values, gain_vector):
    widened = row_values.astype(jnp.float32)
    inverse = lax.rsqrt(jnp.mean(widened * widened, axis=-1, keepdims=True) + 1e-06)
    return (widened * inverse * gain_vector).astype(jnp.bfloat16)


def swap(array, axes, distance, count):
    return lax.ppermute(array, axes, [(i, i ^ distance) for i in range(count)])


def attend(query_norm, keys, values, origins, forget_cum):
    rows, head_count, head_size = query_norm.shape
    blocks = keys.shape[0]
    first_query = lax.axis_index("ep") * rows
    query_positions = first_query + lax.iota(jnp.int32, rows)
    query_cum = lax.dynamic_slice_in_dim(forget_cum, first_query, rows, 0).T
    positions = (origins[:, None] * rows + lax.iota(jnp.int32, rows)[None, :]).reshape(-1)
    key_cum = jnp.concatenate(
        [lax.dynamic_slice_in_dim(forget_cum, origins[b] * rows, rows, 0) for b in range(blocks)]
    ).T
    key_part = keys.reshape(blocks * rows, head_count, head_size)
    value_part = values.reshape(blocks * rows, head_count, head_size)
    scores = jnp.einsum("qhd,khd->hqk", query_norm, key_part, preferred_element_type=jnp.float32)
    scores = scores * head_size ** (-0.5) + query_cum[:, :, None] - key_cum[:, None, :]
    allowed = (positions[None, :] <= query_positions[:, None])[None]
    scores = jnp.where(allowed, scores, -1e30)
    best = jnp.max(scores, axis=2)
    weights = jnp.where(allowed, jnp.exp(scores - best[:, :, None]), 0.0)
    denominator = jnp.sum(weights, axis=2)
    product = jnp.einsum(
        "hqk,khd->hqd",
        weights.astype(jnp.bfloat16),
        value_part,
        preferred_element_type=jnp.float32,
    )
    return (product / denominator[:, :, None]).transpose(1, 0, 2).astype(jnp.bfloat16)


def expert_body(x_ref, gate_ref, up_ref, down_ref, out_ref, grouped, produced, *, experts):
    expert = pl.program_id(0)
    rows, width = x_ref.shape
    per = rows // experts
    chunk = min(width, 1024)

    def source_of(place):
        owner = place // per
        within = place % per
        return (within // CAP) * (experts * CAP) + owner * CAP + within % CAP

    first = lax.broadcasted_iota(jnp.int32, (rows, rows), 0)
    second = lax.broadcasted_iota(jnp.int32, (rows, rows), 1)

    @pl.when(expert == 0)
    def _():
        order = (source_of(first) == second).astype(jnp.float32).astype(jnp.bfloat16)
        for low in range(0, width, chunk):
            piece = jnp.dot(order, x_ref[:, low : low + chunk], preferred_element_type=jnp.float32)
            grouped[:, low : low + chunk] = piece.astype(jnp.bfloat16)

    start = pl.multiple_of(expert * per, per)
    x = grouped[pl.ds(start, per), :]
    gate = jnp.dot(x, gate_ref[0], preferred_element_type=jnp.float32)
    upward = jnp.dot(x, up_ref[0], preferred_element_type=jnp.float32)
    hidden = (jax.nn.silu(gate) * upward).astype(jnp.bfloat16)
    made = jnp.dot(hidden, down_ref[0], preferred_element_type=jnp.float32)
    produced[pl.ds(start, per), :] = made.astype(jnp.bfloat16)

    @pl.when(expert == experts - 1)
    def _():
        order = (source_of(second) == first).astype(jnp.float32).astype(jnp.bfloat16)
        for low in range(0, width, chunk):
            piece = jnp.dot(
                order, produced[:, low : low + chunk], preferred_element_type=jnp.float32
            )
            out_ref[:, low : low + chunk] = piece.astype(jnp.bfloat16)


def run_experts(arrived, gate, up, down, first_expert, experts):
    rows, width = arrived.shape
    hidden = gate.shape[2]
    whole = pl.BlockSpec((rows, width), lambda e: (0, 0))
    return pl.pallas_call(
        functools.partial(expert_body, experts=experts),
        grid=(experts,),
        in_specs=[
            whole,
            pl.BlockSpec((1, width, hidden), lambda e: (e + first_expert, 0, 0)),
            pl.BlockSpec((1, width, hidden), lambda e: (e + first_expert, 0, 0)),
            pl.BlockSpec((1, hidden, width), lambda e: (e + first_expert, 0, 0)),
        ],
        out_specs=whole,
        out_shape=jax.ShapeDtypeStruct((rows, width), jnp.bfloat16),
        scratch_shapes=[pltpu.VMEM((rows, width), jnp.bfloat16)] * 2,
        compiler_params=pltpu.CompilerParams(
            dimension_semantics=("arbitrary",), vmem_limit_bytes=44 * 1024 * 1024
        ),
        cost_estimate=pl.CostEstimate(
            flops=6 * rows * width * hidden,
            transcendentals=rows * hidden,
            bytes_accessed=6 * experts * width * hidden,
        ),
        name=f"experts_{first_expert}",
    )(arrived, gate, up, down)


def dispatch_body(token_ref, gain_ref, slot_ref, normed_ref, *out_refs):
    normed = rms_rows(token_ref[...], gain_ref[...])
    normed_ref[...] = normed
    tokens, width = normed.shape
    chunk = min(width, 1024)
    for number, out_ref in enumerate(out_refs):
        slots = out_ref.shape[0]
        places = lax.broadcasted_iota(jnp.int32, (slots, tokens), 0) + number * slots
        chosen = places == slot_ref[0:1, :]
        for k in range(1, slot_ref.shape[0]):
            chosen = jnp.logical_or(chosen, places == slot_ref[k : k + 1, :])
        chosen = chosen.astype(jnp.float32).astype(jnp.bfloat16)
        for low in range(0, width, chunk):
            piece = jnp.dot(
                chosen, normed_ref[:, low : low + chunk], preferred_element_type=jnp.float32
            )
            out_ref[:, low : low + chunk] = piece.astype(jnp.bfloat16)


def dispatch(tokens, gain, slot_rows, chunks, slots):
    row_count, width = tokens.shape
    shapes = [jax.ShapeDtypeStruct((row_count, width), jnp.bfloat16)]
    shapes += [jax.ShapeDtypeStruct((slots, width), jnp.bfloat16)] * chunks
    return pl.pallas_call(
        dispatch_body,
        out_shape=shapes,
        compiler_params=pltpu.CompilerParams(vmem_limit_bytes=24 * 1024 * 1024),
        name="dispatch",
    )(tokens, gain[None], slot_rows)


def shared_body(normed_ref, *refs):
    part_refs, out_ref = refs[:-1], refs[-1]
    part_width = part_refs[0].shape[1] // 3
    width = normed_ref.shape[1]
    chunk = min(width, 1024)
    contract = (((1,), (1,)), ((), ()))
    normed = normed_ref[...]
    hiddens = []
    for part_ref in part_refs:
        gate = lax.dot_general(
            normed, part_ref[0, :part_width], contract, preferred_element_type=jnp.float32
        )
        upward = lax.dot_general(
            normed,
            part_ref[0, part_width : 2 * part_width],
            contract,
            preferred_element_type=jnp.float32,
        )
        hiddens.append((jax.nn.silu(gate) * upward).astype(jnp.bfloat16))
    for low in range(0, width, chunk):
        total = jnp.zeros((normed.shape[0], chunk), jnp.float32)
        for hidden, part_ref in zip(hiddens, part_refs):
            partial = jnp.dot(
                hidden,
                part_ref[0, 2 * part_width :, low : low + chunk],
                preferred_element_type=jnp.float32,
            )
            total = total + partial.astype(jnp.bfloat16).astype(jnp.float32)
        out_ref[:, low : low + chunk] = total.astype(jnp.bfloat16)


def run_shared(normed, parts):
    return pl.pallas_call(
        shared_body,
        out_shape=jax.ShapeDtypeStruct(normed.shape, jnp.bfloat16),
        compiler_params=pltpu.CompilerParams(vmem_limit_bytes=24 * 1024 * 1024),
        name="shared",
    )(normed, *parts)


def combine_body(slot_ref, weight_ref, shared_ref, *refs):
    returned_refs, out_ref = refs[:-1], refs[-1]
    tokens, slots = slot_ref.shape[0], returned_refs[0].shape[0]
    total = shared_ref[...].astype(jnp.float32)
    places = lax.broadcasted_iota(jnp.int32, (tokens, slots), 1)
    routed = jnp.zeros_like(total)
    for k in range(slot_ref.shape[1]):
        picked = jnp.zeros_like(total)
        for number, returned_ref in enumerate(returned_refs):
            chosen = places + number * slots == slot_ref[:, k : k + 1]
            chosen = chosen.astype(jnp.float32).astype(jnp.bfloat16)
            picked = picked + jnp.dot(
                chosen, returned_ref[...], preferred_element_type=jnp.float32
            )
        routed = routed + weight_ref[:, k : k + 1] * picked
    out_ref[...] = (total + routed).astype(jnp.bfloat16)


def combine(slots, weights, shared_out, returned):
    tokens, width = shared_out.shape
    chunk = min(width, 1024)
    small = pl.BlockSpec(slots.shape, lambda c: (0, 0))
    return pl.pallas_call(
        combine_body,
        grid=(width // chunk,),
        in_specs=[small, small, pl.BlockSpec((tokens, chunk), lambda c: (0, c))]
        + [pl.BlockSpec((r.shape[0], chunk), lambda c: (0, c)) for r in returned],
        out_specs=pl.BlockSpec((tokens, chunk), lambda c: (0, c)),
        out_shape=jax.ShapeDtypeStruct((tokens, width), jnp.bfloat16),
        compiler_params=pltpu.CompilerParams(
            dimension_semantics=("arbitrary",), vmem_limit_bytes=16 * 1024 * 1024
        ),
        name="combine",
    )(slots, weights, shared_out, *returned)


def exchange(rows, count):
    blocks = rows.reshape(count, -1, rows.shape[1])
    moved = lax.all_to_all(blocks, GROUP, split_axis=0, concat_axis=0, tiled=True)
    return moved.reshape(rows.shape)


def local(
    queries,
    key_vectors,
    values,
    forget_cum,
    query_gain,
    key_gain,
    tokens,
    norm_gain,
    routes,
    route_weights,
    expert_gate,
    expert_up,
    expert_down,
    shared_gate,
    shared_up,
    shared_down,
):
    ep_size, tp_size = lax.axis_size("ep"), lax.axis_size("tp")
    count = ep_size * tp_size
    local_count = expert_gate.shape[0]
    row_count, width = tokens.shape
    chunks = CHUNKS if local_count % CHUNKS == 0 else 1
    part_experts = local_count // chunks
    part_slots = count * part_experts * CAP

    row_ids = lax.iota(jnp.int32, row_count)
    earlier = row_ids[None, :] < row_ids[:, None]
    slot_columns = []
    for k in range(routes.shape[1]):
        mine = routes[:, k]
        same = jnp.zeros((row_count, row_count), jnp.int32)
        for other in range(routes.shape[1]):
            same = same + (routes[:, other][None, :] == mine[:, None]).astype(jnp.int32)
        rank = jnp.sum(jnp.where(earlier, same, 0), axis=1)
        block = mine // local_count
        place = mine % local_count
        within = (place % part_experts) * CAP + rank
        slot_columns.append(
            (place // part_experts) * part_slots + block * part_experts * CAP + within
        )
    slots = jnp.stack(slot_columns, axis=1)

    normed, *outgoing = dispatch(
        tokens, norm_gain, jnp.stack(slot_columns, axis=0), chunks, part_slots
    )
    arrived = [exchange(rows, count) for rows in outgoing]

    packed = jnp.concatenate([shared_gate.T, shared_up.T, shared_down], axis=0)[None]
    near = 0
    if power_of_two(tp_size) and tp_size > 1:
        parts = [packed]
        near = tp_size // 2
    else:
        gathered = lax.all_gather(packed, "tp", axis=0, tiled=True)
        parts = [gathered[i : i + 1] for i in range(tp_size)]
    if EARLY_SHARED and near:
        parts = parts + [swap(part, "tp", near, tp_size) for part in parts]
        near //= 2

    ep_index = lax.axis_index("ep")
    query_norm = rms_rows(queries, query_gain)
    key_value = jnp.stack([rms_rows(key_vectors, key_gain), values])
    arrived[0], parts, key_value, query_norm = lax.optimization_barrier(
        (arrived[0], parts, key_value, query_norm)
    )
    if power_of_two(ep_size) and ep_size <= 8:
        key_values = [key_value] + [swap(key_value, "ep", s, ep_size) for s in range(1, ep_size)]
        origins = jnp.stack([ep_index ^ s for s in range(ep_size)])
    else:
        every = lax.all_gather(key_value, "ep", axis=0, tiled=False)
        key_values = [every[s] for s in range(ep_size)]
        origins = lax.iota(jnp.int32, ep_size)
    if near:
        parts = parts + [swap(part, "tp", near, tp_size) for part in parts]
        near //= 2

    returned = []
    for number in range(chunks):
        rows = arrived[number]
        made = run_experts(
            rows, expert_gate, expert_up, expert_down, number * part_experts, part_experts
        )
        if number == 0:
            made, parts, key_values = lax.optimization_barrier((made, parts, key_values))
            while near >= 1:
                parts = parts + [swap(part, "tp", near, tp_size) for part in parts]
                near //= 2
        returned.append(made)
    returned = [exchange(rows, count) for rows in returned]
    attended = attend(
        query_norm,
        jnp.stack([kv[0] for kv in key_values]),
        jnp.stack([kv[1] for kv in key_values]),
        origins,
        forget_cum,
    )
    shared_out = run_shared(normed, parts)
    return attended, combine(slots, route_weights, shared_out, returned)


def solution(mesh):
    placed = (
        P(("grp", "ep"), "tp", None),
        P(("grp", "ep"), "tp", None),
        P(("grp", "ep"), "tp", None),
        P("grp", "tp"),
        P(),
        P(),
        P(("grp", "ep", "tp"), None),
        P(),
        P(("grp", "ep", "tp"), None),
        P(("grp", "ep", "tp"), None),
        P(("ep", "tp"), None, None),
        P(("ep", "tp"), None, None),
        P(("ep", "tp"), None, None),
        P(None, "tp"),
        P(None, "tp"),
        P("tp", None),
    )
    return jax.shard_map(
        local,
        mesh=mesh,
        in_specs=placed,
        out_specs=(P(("grp", "ep"), "tp", None), P(("grp", "ep", "tp"), None)),
        check_vma=False,
    )
```
